32 devices in a mesh: sp: 8 (over z, x), tp: 4 (over y, core).
Axes of the slice: x: 2, y: 2, z: 4, core: 2. Of those that a mesh axis runs over, the one named last changes fastest.
Arguments:
- resid: bfloat16 [2048, 2048], P('sp'), may hold values from -6 to 6
- query_one: bfloat16 [2048, 1024], P('sp', 'tp'), may hold values from -400 to 400
- query_two: bfloat16 [2048, 1024], P('sp', 'tp'), may hold values from -400 to 400
- key_one: bfloat16 [2048, 1024], P('sp', 'tp'), may hold values from -8 to 8
- key_two: bfloat16 [2048, 1024], P('sp', 'tp'), may hold values from -8 to 8
- values: bfloat16 [2048, 2048], P('sp', 'tp'), may hold values from -6 to 6
- documents: int32 [2048], P('sp'), may hold values from 0 to 1, never falling along the last dimension, each value on 1 to 1280 neighbouring positions
- mix_lambda: float32 [16], P('tp'), may hold values from 0.3 to 0.8
- head_gain: float32 [128], replicated, may hold values from 0.1 to 1.9
- out_weight: bfloat16 [2048, 2048], P('tp'), may hold values from -0.125 to 0.125
- ffn_gain: float32 [2048], replicated, may hold values from 0.1 to 1.9
- routes: int32 [2048, 4], P('sp'), may hold values from 0 to 31, all different within a row; in each aligned block of 256 rows (0 to 255, 256 to 511, ...) at most 64 rows name the same one
- route_weight: float32 [2048, 4], P('sp'), may hold values from 0.2 to 0.9
- expert_gate: bfloat16 [32, 2048, 512], P(('sp', 'tp')), may hold values from -0.125 to 0.125
- expert_up: bfloat16 [32, 2048, 512], P(('sp', 'tp')), may hold values from -0.125 to 0.125
- expert_down: bfloat16 [32, 512, 2048], P(('sp', 'tp')), may hold values from -0.25 to 0.25
- shared_gate: bfloat16 [2048, 512], P(None, 'tp'), may hold values from -0.125 to 0.125
- shared_up: bfloat16 [2048, 512], P(None, 'tp'), may hold values from -0.125 to 0.125
- shared_down: bfloat16 [512, 2048], P('tp'), may hold values from -0.25 to 0.25
Outputs:
- layer_out: bfloat16 [2048, 2048], P(('sp', 'tp'))
The draws below stay inside these ranges and needn't reach their ends.
Inputs may be any that keep to these rules, and one draw needn't show every extreme that they name: `documents`: document numbers never fall along the positions; each document has 1 to 1280 positions and one has exactly 1280. `routes`: A row names 4 different experts. In each aligned block of 256 rows no expert is named by more than 64 rows, a bound that some block reaches.
All inputs are finite; a program needn't handle non-finite values.
Results may differ from the reference program's by a relative error of at most 0.018.
Values may be sent and summed in bfloat16 or wider, within the bound.
A program may use at most 128 MiB of HBM per device.

```python
import math
from functools import partial
import jax
import jax.numpy as jnp
import numpy as np
from jax import lax

D = 2048
HEADS = 16
HEAD_DIM = 64
VAL_DIM = 128
EXP_FF = 512
SHARED_FF = 512
TOP = 4
TOK_DEV = 256
TOKENS = 2048
EXPERTS = 32
CAP = 64
DOC_COUNT = 2
DOC_MOST = 1280
N_SP = 8
N_TP = 4


def query_key_pair(key, which):
    base = jax.random.fold_in(key, 101 + which)
    key_query, key_keys = jax.random.split(base, 2)
    shape = (TOKENS, HEADS, HEAD_DIM)
    queries = jnp.clip(jax.random.normal(key_query, shape, jnp.float32) * 1.32, -8.0, 8.0)
    keyed = jnp.clip(jax.random.normal(key_keys, shape, jnp.float32) * 1.32, -8.0, 8.0)
    return (queries.reshape(TOKENS, HEADS * HEAD_DIM), keyed.reshape(TOKENS, HEADS * HEAD_DIM))


def draw_query_one(key, part):
    return query_key_pair(key, 1)[0].astype(jnp.bfloat16)


def draw_key_one(key, part):
    return query_key_pair(key, 1)[1].astype(jnp.bfloat16)


def draw_query_two(key, part):
    return query_key_pair(key, 2)[0].astype(jnp.bfloat16)


def draw_key_two(key, part):
    return query_key_pair(key, 2)[1].astype(jnp.bfloat16)


def steps_of(key, shape, shards, smallest, top_value):
    def one(position, parts):
        draws = jax.random.uniform(jax.random.fold_in(jax.random.fold_in(key, 6), position), (parts,), jnp.float32, smallest / len(shards), top_value / len(shards))
        return jnp.repeat(jnp.exp(draws), shape[position] // parts).reshape((-1,) + (1,) * (len(shape) - position - 1))

    level = one(*shards[0])
    for cut in shards[1:]:
        level = level * one(*cut)
    return level


def split_up(number_of, total, limit, lean):
    loads = [(1 << 20) // math.isqrt(rank ** lean) + 1 for rank in range(2, number_of + 1)]
    surplus, holding = total - limit - (number_of - 1), [1] * (number_of - 1)
    while surplus > 0:
        movable = [i for i in range(number_of - 1) if holding[i] < limit]
        whole, remaining = sum([loads[i] for i in movable]), surplus
        for i in movable:
            extra = min(limit - holding[i], max(1, remaining * loads[i] // whole), surplus)
            holding[i] = holding[i] + extra
            surplus = surplus - extra
    return np.array([limit] + holding)


def ragged(rng, amount, total, limit, skew):
    if amount == 2:
        one = jax.random.randint(rng, (), max(1, total - limit), min(limit, total - 1) + 1)
        return jnp.stack([one, total - one])
    sizes = jnp.asarray(split_up(amount, total, limit, skew), jnp.int32)
    twos = (amount - 1) // 2
    giver, taker = sizes[1:1 + 2 * twos:2], sizes[2:2 + 2 * twos:2]
    room = jnp.minimum(giver - 1, limit - taker)
    moved = jax.random.randint(jax.random.fold_in(rng, 1), (twos,), 0, 1 << 20) % (room + 1)
    sizes = sizes.at[1:1 + 2 * twos:2].set(giver - moved).at[2:2 + 2 * twos:2].set(taker + moved)
    return sizes[jax.random.permutation(jax.random.fold_in(rng, 2), amount)]


def deal_out(key, own, number, rows, count, top, most, lean):
    order = jax.random.permutation(key, count)
    packed, usual = load_shares(count, rows * top, most, lean, True), load_shares(count, rows * top, most, lean, False)
    places = jnp.arange(count)

    def named(tallies, offset_by):
        used = int((tallies > 0).sum())
        fixed = max(1, used // 4)
        shifted = fixed + (places - fixed + offset_by * (used - fixed)) % max(1, count - fixed)
        return jnp.zeros((count,), jnp.int32).at[order[jnp.where(places < fixed, places, shifted)]].set(jnp.asarray(tallies, jnp.int32))

    tallies = jnp.where(number % 4 == 0, named(packed, number // 4), named(usual, number - number // 4 - 1))
    mixed = jax.random.permutation(jax.random.fold_in(own, 3), count)
    giver, taker = mixed[0:count // 2 * 2:2], mixed[1:count // 2 * 2:2]
    slack = jnp.minimum(tallies[giver] - 1, most - tallies[taker]) // 2
    slack = jnp.where((giver == order[0]) | (taker == order[0]) | (tallies[taker] == 0), 0, jnp.maximum(slack, 0))
    shifted = jax.random.randint(jax.random.fold_in(own, 4), (count // 2,), 0, 1 << 20) % (slack + 1)
    tallies = tallies.at[giver].add(-shifted).at[taker].add(shifted)
    labels = jnp.searchsorted(jnp.cumsum(tallies), jnp.arange(rows * top), side="right").astype(jnp.int32)
    listing = labels.reshape(top, rows).T
    listing = listing[jax.random.permutation(jax.random.fold_in(own, 1), rows)]
    offset_by = jax.random.randint(jax.random.fold_in(own, 2), (rows, 1), 0, top)
    return jnp.take_along_axis(listing, (jnp.arange(top)[None, :] + offset_by) % top, axis=1)


def load_shares(amount, total, bound, lean, full):
    portions = [(1 << 20) // math.isqrt(rank ** lean) + 1 for rank in range(1, amount + 1)]
    largest = bound if full else min(bound, max(-(-total // amount), total * portions[0] // sum(portions)))
    least = 1 if total - largest >= amount - 1 else 0
    counts, spare = [largest] + [least] * (amount - 1), total - largest - least * (amount - 1)
    while spare > 0:
        free = [i for i in range(1, amount) if counts[i] < largest] or [i for i in range(1, amount) if counts[i] < bound]
        mass, left = sum([portions[i] for i in free]), spare
        for i in free:
            addition = min(bound - counts[i], max(1, left * portions[i] // mass), spare)
            counts[i] = counts[i] + addition
            spare = spare - addition
    return np.array(counts)


def gaussian(rng, shape, deviation, reach, shards=(), held_as=jnp.bfloat16):
    entries = jax.random.normal(rng, shape, jnp.float32) * deviation
    if len(shards) > 0:
        entries = steps_of(rng, shape, shards, -0.22, 0.18) * entries
    return jnp.clip(entries, min=-reach, max=reach).astype(held_as)


def setup_inputs(seed: int = 0) -> dict:
    streams_of = jax.random.split(jax.random.key(seed), 20)
    resid = gaussian(streams_of[0], (TOKENS, D), 1.0, 6.0, ((0, 8),))
    query_one = draw_query_one(jax.random.fold_in(streams_of[19], 71), 0)
    query_two = draw_query_two(jax.random.fold_in(streams_of[19], 71), 0)
    key_one = draw_key_one(jax.random.fold_in(streams_of[19], 71), 0)
    key_two = draw_key_two(jax.random.fold_in(streams_of[19], 71), 0)
    values = gaussian(streams_of[5], (TOKENS, HEADS * VAL_DIM), 1.0, 6.0, ((0, 8), (1, 4)))
    documents = jnp.searchsorted(jnp.cumsum(ragged(streams_of[6], DOC_COUNT, TOKENS, DOC_MOST, 0)), jnp.arange(TOKENS), side="right").astype(jnp.int32)
    mix_lambda = jnp.clip(0.3 + 0.5 * jax.random.uniform(streams_of[7], (HEADS,), jnp.float32) ** steps_of(streams_of[7], (HEADS,), ((0, 4),), -0.2, 0.2), 0.3, 0.8)
    head_gain = jnp.clip(1.0 + 0.18 * jax.random.normal(streams_of[8], (VAL_DIM,), jnp.float32), 0.1, 1.9)
    out_weight = gaussian(streams_of[9], (HEADS * VAL_DIM, D), (HEADS * VAL_DIM) ** -0.5, 0.125, ((0, 4),))
    ffn_gain = jnp.clip(1.0 + 0.18 * jax.random.normal(streams_of[10], (D,), jnp.float32), 0.1, 1.9)
    routes_keys = jax.random.split(jax.random.fold_in(streams_of[11], 1), TOKENS // TOK_DEV)
    routes_turns = jax.random.permutation(jax.random.fold_in(streams_of[11], 3), TOKENS // TOK_DEV)
    routes = jax.vmap(lambda own, number: deal_out(jax.random.fold_in(streams_of[11], 2), own, number, TOK_DEV, EXPERTS, TOP, CAP, 2))(routes_keys, routes_turns).reshape((TOKENS, TOP))
    route_weight = jnp.clip(0.2 + 0.7 * jax.random.uniform(streams_of[12], (TOKENS, TOP), jnp.float32) ** steps_of(streams_of[12], (TOKENS, TOP), ((0, 8),), -0.2, 0.2), 0.2, 0.9)
    expert_gate = gaussian(streams_of[13], (EXPERTS, D, EXP_FF), D ** -0.5, 0.125, ((0, 32),))
    expert_up = gaussian(streams_of[14], (EXPERTS, D, EXP_FF), D ** -0.5, 0.125, ((0, 32),))
    expert_down = gaussian(streams_of[15], (EXPERTS, EXP_FF, D), EXP_FF ** -0.5, 0.25, ((0, 32),))
    shared_gate = gaussian(streams_of[16], (D, SHARED_FF), D ** -0.5, 0.125, ((1, 4),))
    shared_up = gaussian(streams_of[17], (D, SHARED_FF), D ** -0.5, 0.125, ((1, 4),))
    shared_down = gaussian(streams_of[18], (SHARED_FF, D), SHARED_FF ** -0.5, 0.25, ((0, 4),))
    return dict(resid=resid, query_one=query_one, query_two=query_two, key_one=key_one, key_two=key_two, values=values, documents=documents, mix_lambda=mix_lambda, head_gain=head_gain, out_weight=out_weight, ffn_gain=ffn_gain, routes=routes, route_weight=route_weight, expert_gate=expert_gate, expert_up=expert_up, expert_down=expert_down, shared_gate=shared_gate, shared_up=shared_up, shared_down=shared_down)


HEAD_SCALE = 0.8

def head_rows(inputs, documents, head_gain):
    query_first, query_second, key_first, key_second, value_rows, lambda_value = inputs
    seq_len = key_first.shape[0]
    key_pos = jnp.arange(seq_len, dtype=jnp.int32)
    score_scale = HEAD_DIM ** (-0.5)

    def query_block(block_idx):
        offset = block_idx * TOK_DEV
        query_pos = offset + jnp.arange(TOK_DEV, dtype=jnp.int32)
        query_docs = lax.dynamic_slice_in_dim(documents, offset, TOK_DEV, 0)
        allowed = (key_pos[None, :] <= query_pos[:, None]) & (documents[None, :] == query_docs[:, None])

        def probs(queries, keys):
            block_query = lax.dynamic_slice_in_dim(queries, offset, TOK_DEV, 0)
            raw = jnp.dot(block_query, keys.T, preferred_element_type=jnp.float32) * score_scale
            masked = jnp.where(allowed, raw, -jnp.inf)
            top_row = lax.optimization_barrier(jnp.max(masked, axis=-1, keepdims=True))
            exp_terms = jnp.where(allowed, jnp.exp(masked - top_row), 0.0)
            return exp_terms / lax.optimization_barrier(jnp.sum(exp_terms, axis=-1, keepdims=True))
        weights = (probs(query_first, key_first) - lambda_value * probs(query_second, key_second)).astype(jnp.bfloat16)
        return jnp.dot(weights, value_rows, preferred_element_type=jnp.float32)
    blocks = lax.map(query_block, jnp.arange(seq_len // TOK_DEV, dtype=jnp.int32))
    head_out = blocks.reshape(seq_len, VAL_DIM)
    scaled = head_out * lax.rsqrt(lax.optimization_barrier(jnp.mean(head_out * head_out, axis=-1, keepdims=True)) + 1e-05)
    return (scaled * head_gain * HEAD_SCALE).astype(jnp.bfloat16)

def by_head(array_in, width):
    return array_in.reshape(TOKENS, HEADS, width).transpose(1, 0, 2)

def reference(resid, query_one, query_two, key_one, key_two, values, documents, mix_lambda, head_gain, out_weight, ffn_gain, routes, route_weight, expert_gate, expert_up, expert_down, shared_gate, shared_up, shared_down):
    head_fn = partial(head_rows, documents=documents, head_gain=head_gain)
    heads_out = lax.map(head_fn, (by_head(query_one, HEAD_DIM), by_head(query_two, HEAD_DIM), by_head(key_one, HEAD_DIM), by_head(key_two, HEAD_DIM), by_head(values, VAL_DIM), mix_lambda))
    attn_rows = heads_out.transpose(1, 0, 2).reshape(TOKENS, HEADS * VAL_DIM)
    group_cols = HEADS // N_TP * VAL_DIM
    projected = jnp.zeros((TOKENS, D), jnp.float32)
    for group in range(N_TP):
        part_sum = jnp.dot(attn_rows[:, group * group_cols:(group + 1) * group_cols], out_weight[group * group_cols:(group + 1) * group_cols], preferred_element_type=jnp.float32)
        projected = projected + lax.optimization_barrier(part_sum.astype(jnp.bfloat16)).astype(jnp.float32)
    mixed = resid.astype(jnp.float32) + projected
    normed = (mixed * lax.rsqrt(lax.optimization_barrier(jnp.mean(mixed * mixed, axis=-1, keepdims=True)) + 1e-06) * ffn_gain).astype(jnp.bfloat16)
    assign_total = TOKENS * TOP
    flat_expert = routes.reshape(assign_total)
    flat_weight = route_weight.reshape(assign_total)
    assign_token = jnp.arange(assign_total, dtype=jnp.int32) // TOP
    assign_block = jnp.arange(assign_total, dtype=jnp.int32) // (TOK_DEV * TOP)
    one_hot = (flat_expert[:, None] == jnp.arange(EXPERTS, dtype=jnp.int32)[None, :]).astype(jnp.int32)
    running = jnp.cumsum(one_hot.reshape(N_SP, TOK_DEV * TOP, EXPERTS), axis=1).reshape(assign_total, EXPERTS)
    slot_rank = lax.optimization_barrier(jnp.sum(running * one_hot, axis=1)) - 1
    slot_id = (flat_expert * (N_SP * CAP) + assign_block * CAP + slot_rank).astype(jnp.int32)
    slot_token = jnp.full((EXPERTS * N_SP * CAP,), TOKENS, jnp.int32).at[slot_id].set(assign_token)
    padded = jnp.concatenate([normed, jnp.zeros((1, D), jnp.bfloat16)], axis=0)

    def run_expert(inputs):
        token_idx, gate_w, up_w, down_w = inputs
        rows_in = padded[token_idx]
        gate_part = jnp.dot(rows_in, gate_w, preferred_element_type=jnp.float32)
        up_part = jnp.dot(rows_in, up_w, preferred_element_type=jnp.float32)
        hidden = (jax.nn.silu(gate_part) * up_part).astype(jnp.bfloat16)
        return jnp.dot(hidden, down_w, preferred_element_type=jnp.float32).astype(jnp.bfloat16)
    expert_rows = lax.map(run_expert, (slot_token.reshape(EXPERTS, N_SP * CAP), expert_gate, expert_up, expert_down))
    flat_rows = expert_rows.reshape(EXPERTS * N_SP * CAP, D)
    weighted = (flat_rows[slot_id].astype(jnp.float32) * flat_weight[:, None]).reshape(TOKENS, TOP, D)
    expert_group = routes % N_TP
    shared_act = (jax.nn.silu(jnp.dot(normed, shared_gate, preferred_element_type=jnp.float32)) * jnp.dot(normed, shared_up, preferred_element_type=jnp.float32)).astype(jnp.bfloat16)
    shared_cols = SHARED_FF // N_TP
    ffn_total = jnp.zeros((TOKENS, D), jnp.float32)
    for group in range(N_TP):
        chosen = (expert_group == group).astype(jnp.float32)
        routed = lax.optimization_barrier(jnp.sum(weighted * chosen[:, :, None], axis=1))
        shared_part = jnp.dot(shared_act[:, group * shared_cols:(group + 1) * shared_cols], shared_down[group * shared_cols:(group + 1) * shared_cols], preferred_element_type=jnp.float32)
        ffn_total = ffn_total + lax.optimization_barrier((routed + shared_part).astype(jnp.bfloat16)).astype(jnp.float32)
    return (mixed + ffn_total).astype(jnp.bfloat16)
```

```python
import functools

import jax
import jax.numpy as jnp
from jax import lax
from jax.experimental import pallas as pl
from jax.experimental.pallas import tpu as pltpu
from jax.sharding import PartitionSpec as P

NEG_FILL = -1e30
HEAD_SCALE = 0.8


def rms_scale(values_in, eps_value):
    return lax.rsqrt(jnp.mean(values_in * values_in, axis=-1, keepdims=True) + eps_value)


def row_width(count):
    width = 1
    while (2 * width) * (2 * width) <= count:
        width *= 2
    return width if count % width == 0 else 1


def gather_kernel(count, wide, k1, k2, val, doc, k1_all, k2_all, val_all, doc_all,
                  own_sem, z_send, z_recv, x_send, x_recv, d_send, d_recv):
    tall = count // wide
    me = lax.axis_index("sp")
    row, col = me // wide, me % wide
    pieces = ((k1, k1_all), (k2, k2_all), (val, val_all))

    barrier = pltpu.get_barrier_semaphore()
    for off in range(1, count):
        pl.semaphore_signal(
            barrier, inc=1, device_id={"sp": lax.rem(me + off, count)},
            device_id_type=pl.DeviceIdType.MESH,
        )
    pl.semaphore_wait(barrier, count - 1)

    def remote(src, dst, send, recv, target):
        return pltpu.make_async_remote_copy(
            src_ref=src, dst_ref=dst, send_sem=send, recv_sem=recv,
            device_id={"sp": target}, device_id_type=pl.DeviceIdType.MESH,
        )

    def hop(way, hops, piece):
        src, everything = pieces[piece]
        step = 1 if way == 0 else -1
        origin = (row + step - step * hops) * wide + col
        slot = everything.at[origin]
        source = src if hops == 1 else slot
        return remote(source, slot, z_send.at[way, hops, piece], z_recv.at[way, hops, piece],
                      me + step * wide)

    def arrived_hop(way, hops, piece):
        everything = pieces[piece][1]
        step = 1 if way == 0 else -1
        slot = everything.at[me - step * hops * wide]
        return remote(slot, slot, z_send.at[way, hops, piece], z_recv.at[way, hops, piece],
                      me - step * wide)

    def across(way, hops, piece, off, landing):
        src, everything = pieces[piece]
        step = 1 if way == 0 else -1
        from_col = lax.rem(col + wide - off, wide) if landing else col
        slot = everything.at[(row - step * hops) * wide + from_col]
        source = src if hops == 0 and not landing else slot
        target = row * wide + (from_col if landing else lax.rem(col + off, wide))
        return remote(source, slot, x_send.at[way, hops, piece, off],
                      x_recv.at[way, hops, piece, off], target)

    offsets = range(1, wide)
    ways = (0, 1)

    def has(way, hops):
        return row >= hops if way == 0 else row + hops < tall

    def open_end(way):
        return row + 1 < tall if way == 0 else row > 0

    doc_copies = [
        remote(doc, doc_all.at[me], d_send.at[off], d_recv.at[off], lax.rem(me + off, count))
        for off in range(1, count)
    ]
    own_copies = [
        pltpu.make_async_copy(src, everything.at[me], own_sem.at[piece])
        for piece, (src, everything) in enumerate(pieces + ((doc, doc_all),))
    ]
    for copy in doc_copies:
        copy.start()
    for piece in range(3):
        for way in ways:
            @pl.when(open_end(way))
            def _(way=way, piece=piece):
                hop(way, 1, piece).start()
        for off in offsets:
            across(0, 0, piece, off, False).start()
    for copy in own_copies:
        copy.start()
    for hops in range(1, tall):
        for piece in range(3):
            for way in ways:
                @pl.when(has(way, hops))
                def _(way=way, piece=piece, hops=hops):
                    arrived_hop(way, hops, piece).wait_recv()
                    if hops + 1 < tall:
                        @pl.when(open_end(way))
                        def _():
                            hop(way, hops + 1, piece).start()
                    for off in offsets:
                        across(way, hops, piece, off, False).start()
    for piece in range(3):
        for off in offsets:
            across(0, 0, piece, off, True).wait_recv()
            across(0, 0, piece, off, False).wait_send()
        for way in ways:
            @pl.when(open_end(way))
            def _(way=way, piece=piece):
                hop(way, 1, piece).wait_send()
    for hops in range(1, tall):
        for piece in range(3):
            for way in ways:
                @pl.when(has(way, hops))
                def _(way=way, piece=piece, hops=hops):
                    if hops + 1 < tall:
                        @pl.when(open_end(way))
                        def _():
                            hop(way, hops + 1, piece).wait_send()
                    for off in offsets:
                        across(way, hops, piece, off, True).wait_recv()
                        across(way, hops, piece, off, False).wait_send()
    for copy in own_copies:
        copy.wait()
    for off in range(1, count):
        sender = lax.rem(me + count - off, count)
        slot = doc_all.at[sender]
        remote(slot, slot, d_send.at[off], d_recv.at[off], sender).wait_recv()
        doc_copies[off - 1].wait_send()


def gather_all(key_one, key_two, values, documents):
    count = lax.axis_size("sp")
    wide = row_width(count)
    tall = count // wide
    dma = pltpu.SemaphoreType.DMA
    rows = key_one.shape[0]
    doc = documents.reshape(1, rows)
    outs = [jax.ShapeDtypeStruct((count,) + a.shape, a.dtype)
            for a in (key_one, key_two, values, doc)]
    vmem = pl.BlockSpec(memory_space=pltpu.VMEM)
    sent = (count - 1) * (key_one.size + key_two.size + values.size) * 2
    return pl.pallas_call(
        functools.partial(gather_kernel, count, wide),
        out_shape=outs,
        in_specs=[vmem] * 4,
        out_specs=[vmem] * 4,
        scratch_shapes=[
            dma((4,)), dma((2, tall, 3)), dma((2, tall, 3)),
            dma((2, tall, 3, wide)), dma((2, tall, 3, wide)), dma((count,)), dma((count,)),
        ],
        compiler_params=pltpu.CompilerParams(collective_id=0, has_side_effects=True,
                                             vmem_limit_bytes=40 * 1024 * 1024),
        cost_estimate=pl.CostEstimate(flops=0, bytes_accessed=sent, transcendentals=0),
        name="gather_keys",
    )(key_one, key_two, values, doc)


def local(
    resid,
    query_one,
    query_two,
    key_one,
    key_two,
    values,
    documents,
    mix_lambda,
    head_gain,
    out_weight,
    ffn_gain,
    routes,
    route_weight,
    expert_gate,
    expert_up,
    expert_down,
    shared_gate,
    shared_up,
    shared_down,
):
    tok_rows = query_one.shape[0]
    head_count = mix_lambda.shape[0]
    head_width = query_one.shape[1] // head_count
    value_width = values.shape[1] // head_count
    model_width = resid.shape[1]
    score_scale = head_width ** (-0.5)
    seq_size = lax.axis_size("sp")
    tp_size = lax.axis_size("tp")
    query_pos = lax.axis_index("sp") * tok_rows + jnp.arange(tok_rows, dtype=jnp.int32)
    query_first = query_one.reshape(tok_rows, head_count, head_width)
    query_second = query_two.reshape(tok_rows, head_count, head_width)
    lambda_col = mix_lambda[:, None, None]
    key_first, key_second, value_block, key_docs = gather_all(
        key_one, key_two, values, documents
    )
    key_total = seq_size * tok_rows
    key_docs = key_docs.reshape(key_total)
    key_pos = jnp.arange(key_total, dtype=jnp.int32)
    allowed = (
        (key_pos[None, :] <= query_pos[:, None]) & (key_docs[None, :] == documents[:, None])
    )[None]

    def probs(query_block, key_block):
        keyed = key_block.reshape(key_total, head_count, head_width)
        raw = (
            jnp.einsum("qhd,khd->hqk", query_block, keyed, preferred_element_type=jnp.float32)
            * score_scale
        )
        masked = jnp.where(allowed, raw, NEG_FILL)
        fresh = jnp.exp(masked - jnp.max(masked, axis=-1, keepdims=True))
        return fresh / jnp.sum(fresh, axis=-1, keepdims=True)

    weights = (
        probs(query_first, key_first) - lambda_col * probs(query_second, key_second)
    ).astype(jnp.bfloat16)
    valued = value_block.reshape(key_total, head_count, value_width)
    head_out = jnp.einsum("hqk,khv->hqv", weights, valued, preferred_element_type=jnp.float32)
    normed_heads = (head_out * rms_scale(head_out, 1e-05) * head_gain * HEAD_SCALE).astype(
        jnp.bfloat16
    )
    attn_rows = normed_heads.transpose(1, 0, 2).reshape(tok_rows, head_count * value_width)
    share_rows = tok_rows // tp_size
    own_start = lax.axis_index("tp") * share_rows
    proj_term = jnp.dot(attn_rows, out_weight, preferred_element_type=jnp.float32)
    projected = lax.psum(proj_term.astype(jnp.bfloat16), "tp").astype(jnp.float32)
    mixed_all = resid.astype(jnp.float32) + projected
    normed_all = (mixed_all * rms_scale(mixed_all, 1e-06) * ffn_gain).astype(jnp.bfloat16)
    mixed_own = lax.dynamic_slice_in_dim(mixed_all, own_start, share_rows, 0)
    route_slots = routes.shape[1]
    capacity = max(2, 2 * tok_rows * route_slots // (seq_size * tp_size))
    tp_index = lax.axis_index("tp")
    group_experts = jnp.arange(seq_size, dtype=jnp.int32) * tp_size + tp_index
    named = routes[:, :, None] == group_experts[None, None, :]
    token_weight = jnp.sum(jnp.where(named, route_weight[:, :, None], 0.0), axis=1)
    is_named = jnp.any(named, axis=1)
    token_pos = jnp.arange(tok_rows, dtype=jnp.int32)
    earlier = (token_pos[None, :] < token_pos[:, None]).astype(jnp.bfloat16)
    rank = jnp.dot(earlier, is_named.astype(jnp.bfloat16), preferred_element_type=jnp.float32)
    place = jnp.where(is_named, rank.astype(jnp.int32), -1)
    slot_total = seq_size * capacity
    in_slot = place[:, :, None] == jnp.arange(capacity, dtype=jnp.int32)[None, None, :]
    pick = in_slot.reshape(tok_rows, slot_total).astype(jnp.bfloat16)
    combine = jnp.where(in_slot, token_weight[:, :, None], 0.0).reshape(tok_rows, slot_total)
    combine_high = lax.reduce_precision(combine, 8, 7)
    combine_low = (combine - combine_high).astype(jnp.bfloat16)
    outgoing = lax.dot_general(
        pick, normed_all, (((0,), (0,)), ((), ())), preferred_element_type=jnp.float32
    ).astype(jnp.bfloat16).reshape(seq_size, capacity, model_width)
    arrived = lax.all_to_all(outgoing, "sp", split_axis=0, concat_axis=0, tiled=True)
    item_count = arrived.shape[1]
    flat_rows = arrived.reshape(seq_size * item_count, model_width)
    gate_part = jnp.dot(flat_rows, expert_gate[0], preferred_element_type=jnp.float32)
    up_part = jnp.dot(flat_rows, expert_up[0], preferred_element_type=jnp.float32)
    hidden = (jax.nn.silu(gate_part) * up_part).astype(jnp.bfloat16)
    result = jnp.dot(hidden, expert_down[0], preferred_element_type=jnp.float32).astype(
        jnp.bfloat16
    )
    returned = lax.all_to_all(
        result.reshape(seq_size, item_count, model_width),
        "sp",
        split_axis=0,
        concat_axis=0,
        tiled=True,
    )
    returned_flat = returned.reshape(slot_total, model_width)
    routed = jnp.dot(
        combine_high.astype(jnp.bfloat16), returned_flat, preferred_element_type=jnp.float32
    ) + jnp.dot(combine_low, returned_flat, preferred_element_type=jnp.float32)
    shared_act = (
        jax.nn.silu(jnp.dot(normed_all, shared_gate, preferred_element_type=jnp.float32))
        * jnp.dot(normed_all, shared_up, preferred_element_type=jnp.float32)
    ).astype(jnp.bfloat16)
    shared_out = jnp.dot(shared_act, shared_down, preferred_element_type=jnp.float32)
    ffn_own = lax.psum_scatter(
        (routed + shared_out).astype(jnp.bfloat16), "tp", scatter_dimension=0, tiled=True
    ).astype(jnp.float32)
    return (mixed_own + ffn_own).astype(jnp.bfloat16)


def solution(mesh):
    placed = (
        P("sp", None),
        P("sp", "tp"),
        P("sp", "tp"),
        P("sp", "tp"),
        P("sp", "tp"),
        P("sp", "tp"),
        P("sp"),
        P("tp"),
        P(),
        P("tp", None),
        P(),
        P("sp", None),
        P("sp", None),
        P(("sp", "tp"), None, None),
        P(("sp", "tp"), None, None),
        P(("sp", "tp"), None, None),
        P(None, "tp"),
        P(None, "tp"),
        P("tp", None),
    )
    return jax.shard_map(
        local, mesh=mesh, in_specs=placed, out_specs=P(("sp", "tp"), None), check_vma=False
    )
```

```python
import functools

import jax
import jax.numpy as jnp
from jax import lax
from jax.experimental import pallas as pl
from jax.experimental.pallas import tpu as pltpu
from jax.sharding import PartitionSpec as P

NEG_FILL = -1e30
HEAD_SCALE = 0.8


def rms_scale(values_in, eps_value):
    return lax.rsqrt(jnp.mean(values_in * values_in, axis=-1, keepdims=True) + eps_value)


def row_width(count):
    width = 1
    while (2 * width) * (2 * width) <= count:
        width *= 2
    return width if count % width == 0 else 1


def gather_kernel(count, wide, k1, k2, val, doc, k1_all, k2_all, val_all, doc_all,
                  own_sem, z_send, z_recv, x_send, x_recv, d_send, d_recv):
    tall = count // wide
    me = lax.axis_index("sp")
    row, col = me // wide, me % wide
    pieces = ((k1, k1_all), (k2, k2_all), (val, val_all))

    barrier = pltpu.get_barrier_semaphore()
    for off in range(1, count):
        pl.semaphore_signal(
            barrier, inc=1, device_id={"sp": lax.rem(me + off, count)},
            device_id_type=pl.DeviceIdType.MESH,
        )
    pl.semaphore_wait(barrier, count - 1)

    def remote(src, dst, send, recv, target):
        return pltpu.make_async_remote_copy(
            src_ref=src, dst_ref=dst, send_sem=send, recv_sem=recv,
            device_id={"sp": target}, device_id_type=pl.DeviceIdType.MESH,
        )

    def hop(way, hops, piece):
        src, everything = pieces[piece]
        step = 1 if way == 0 else -1
        origin = (row + step - step * hops) * wide + col
        slot = everything.at[origin]
        source = src if hops == 1 else slot
        return remote(source, slot, z_send.at[way, hops, piece], z_recv.at[way, hops, piece],
                      me + step * wide)

    def arrived_hop(way, hops, piece):
        everything = pieces[piece][1]
        step = 1 if way == 0 else -1
        slot = everything.at[me - step * hops * wide]
        return remote(slot, slot, z_send.at[way, hops, piece], z_recv.at[way, hops, piece],
                      me - step * wide)

    def across(way, hops, piece, off, landing):
        src, everything = pieces[piece]
        step = 1 if way == 0 else -1
        from_col = lax.rem(col + wide - off, wide) if landing else col
        slot = everything.at[(row - step * hops) * wide + from_col]
        source = src if hops == 0 and not landing else slot
        target = row * wide + (from_col if landing else lax.rem(col + off, wide))
        return remote(source, slot, x_send.at[way, hops, piece, off],
                      x_recv.at[way, hops, piece, off], target)

    offsets = range(1, wide)
    ways = (0, 1)

    def has(way, hops):
        return row >= hops if way == 0 else row + hops < tall

    def open_end(way):
        return row + 1 < tall if way == 0 else row > 0

    doc_copies = [
        remote(doc, doc_all.at[me], d_send.at[off], d_recv.at[off], lax.rem(me + off, count))
        for off in range(1, count)
    ]
    own_copies = [
        pltpu.make_async_copy(src, everything.at[me], own_sem.at[piece])
        for piece, (src, everything) in enumerate(pieces + ((doc, doc_all),))
    ]
    for copy in doc_copies:
        copy.start()
    for piece in range(3):
        for way in ways:
            @pl.when(open_end(way))
            def _(way=way, piece=piece):
                hop(way, 1, piece).start()
        for off in offsets:
            across(0, 0, piece, off, False).start()
    for copy in own_copies:
        copy.start()
    for hops in range(1, tall):
        for piece in range(3):
            for way in ways:
                @pl.when(has(way, hops))
                def _(way=way, piece=piece, hops=hops):
                    arrived_hop(way, hops, piece).wait_recv()
                    if hops + 1 < tall:
                        @pl.when(open_end(way))
                        def _():
                            hop(way, hops + 1, piece).start()
                    for off in offsets:
                        across(way, hops, piece, off, False).start()
    for piece in range(3):
        for off in offsets:
            across(0, 0, piece, off, True).wait_recv()
            across(0, 0, piece, off, False).wait_send()
        for way in ways:
            @pl.when(open_end(way))
            def _(way=way, piece=piece):
                hop(way, 1, piece).wait_send()
    for hops in range(1, tall):
        for piece in range(3):
            for way in ways:
                @pl.when(has(way, hops))
                def _(way=way, piece=piece, hops=hops):
                    if hops + 1 < tall:
                        @pl.when(open_end(way))
                        def _():
                            hop(way, hops + 1, piece).wait_send()
                    for off in offsets:
                        across(way, hops, piece, off, True).wait_recv()
                        across(way, hops, piece, off, False).wait_send()
    for copy in own_copies:
        copy.wait()
    for off in range(1, count):
        sender = lax.rem(me + count - off, count)
        slot = doc_all.at[sender]
        remote(slot, slot, d_send.at[off], d_recv.at[off], sender).wait_recv()
        doc_copies[off - 1].wait_send()


def gather_all(key_one, key_two, values, documents):
    count = lax.axis_size("sp")
    wide = row_width(count)
    tall = count // wide
    dma = pltpu.SemaphoreType.DMA
    rows = key_one.shape[0]
    doc = documents.reshape(1, rows)
    outs = [jax.ShapeDtypeStruct((count,) + a.shape, a.dtype)
            for a in (key_one, key_two, values, doc)]
    vmem = pl.BlockSpec(memory_space=pltpu.VMEM)
    sent = (count - 1) * (key_one.size + key_two.size + values.size) * 2
    return pl.pallas_call(
        functools.partial(gather_kernel, count, wide),
        out_shape=outs,
        in_specs=[vmem] * 4,
        out_specs=[vmem] * 4,
        scratch_shapes=[
            dma((4,)), dma((2, tall, 3)), dma((2, tall, 3)),
            dma((2, tall, 3, wide)), dma((2, tall, 3, wide)), dma((count,)), dma((count,)),
        ],
        compiler_params=pltpu.CompilerParams(collective_id=0, has_side_effects=True,
                                             vmem_limit_bytes=40 * 1024 * 1024),
        cost_estimate=pl.CostEstimate(flops=0, bytes_accessed=sent, transcendentals=0),
        name="gather_keys",
    )(key_one, key_two, values, doc)


def swap_kernel(count, spread, src, out, own_sem, send, recv):
    me = lax.axis_index("tp")
    barrier = pltpu.get_barrier_semaphore()
    for off in range(1, count):
        pl.semaphore_signal(
            barrier, inc=1, device_id={"tp": lax.rem(me + off, count)},
            device_id_type=pl.DeviceIdType.MESH,
        )
    pl.semaphore_wait(barrier, count - 1)

    def part(index):
        return src.at[index] if spread else src.at[0]

    copies = []
    for off in range(1, count):
        target = lax.rem(me + off, count)
        copy = pltpu.make_async_remote_copy(
            src_ref=part(target), dst_ref=out.at[me], send_sem=send.at[off],
            recv_sem=recv.at[off], device_id={"tp": target},
            device_id_type=pl.DeviceIdType.MESH,
        )
        copy.start()
        copies.append(copy)
    own = pltpu.make_async_copy(part(me), out.at[me], own_sem.at[0])
    own.start()
    for off in range(1, count):
        sender = lax.rem(me + count - off, count)
        pltpu.make_async_remote_copy(
            src_ref=out.at[sender], dst_ref=out.at[sender], send_sem=send.at[off],
            recv_sem=recv.at[off], device_id={"tp": sender},
            device_id_type=pl.DeviceIdType.MESH,
        ).wait_recv()
        copies[off - 1].wait_send()
    own.wait()


def swap_tp(parts, collective_id):
    count = lax.axis_size("tp")
    dma = pltpu.SemaphoreType.DMA
    vmem = pl.BlockSpec(memory_space=pltpu.VMEM)
    return pl.pallas_call(
        functools.partial(swap_kernel, count, parts.shape[0] == count),
        out_shape=jax.ShapeDtypeStruct((count,) + parts.shape[1:], parts.dtype),
        in_specs=[vmem],
        out_specs=vmem,
        scratch_shapes=[dma((1,)), dma((count,)), dma((count,))],
        compiler_params=pltpu.CompilerParams(collective_id=collective_id, has_side_effects=True),
        name="swap_tp_%d" % collective_id,
    )(parts)


def local(
    resid,
    query_one,
    query_two,
    key_one,
    key_two,
    values,
    documents,
    mix_lambda,
    head_gain,
    out_weight,
    ffn_gain,
    routes,
    route_weight,
    expert_gate,
    expert_up,
    expert_down,
    shared_gate,
    shared_up,
    shared_down,
):
    tok_rows = query_one.shape[0]
    head_count = mix_lambda.shape[0]
    head_width = query_one.shape[1] // head_count
    value_width = values.shape[1] // head_count
    model_width = resid.shape[1]
    score_scale = head_width ** (-0.5)
    seq_size = lax.axis_size("sp")
    tp_size = lax.axis_size("tp")
    query_pos = lax.axis_index("sp") * tok_rows + jnp.arange(tok_rows, dtype=jnp.int32)
    query_first = query_one.reshape(tok_rows, head_count, head_width)
    query_second = query_two.reshape(tok_rows, head_count, head_width)
    lambda_col = mix_lambda[:, None, None]
    key_first, key_second, value_block, key_docs = gather_all(
        key_one, key_two, values, documents
    )
    key_total = seq_size * tok_rows
    key_docs = key_docs.reshape(key_total)
    key_pos = jnp.arange(key_total, dtype=jnp.int32)
    allowed = (
        (key_pos[None, :] <= query_pos[:, None]) & (key_docs[None, :] == documents[:, None])
    )[None]

    def probs(query_block, key_block):
        keyed = key_block.reshape(key_total, head_count, head_width)
        raw = (
            jnp.einsum("qhd,khd->hqk", query_block, keyed, preferred_element_type=jnp.float32)
            * score_scale
        )
        masked = jnp.where(allowed, raw, NEG_FILL)
        fresh = jnp.exp(masked - jnp.max(masked, axis=-1, keepdims=True))
        return fresh / jnp.sum(fresh, axis=-1, keepdims=True)

    weights = (
        probs(query_first, key_first) - lambda_col * probs(query_second, key_second)
    ).astype(jnp.bfloat16)
    valued = value_block.reshape(key_total, head_count, value_width)
    head_out = jnp.einsum("hqk,khv->hqv", weights, valued, preferred_element_type=jnp.float32)
    normed_heads = (head_out * rms_scale(head_out, 1e-05) * head_gain * HEAD_SCALE).astype(
        jnp.bfloat16
    )
    attn_rows = normed_heads.transpose(1, 0, 2).reshape(tok_rows, head_count * value_width)
    share_rows = tok_rows // tp_size
    own_start = lax.axis_index("tp") * share_rows
    proj_term = jnp.dot(attn_rows, out_weight, preferred_element_type=jnp.float32)
    proj_parts = swap_tp(
        proj_term.astype(jnp.bfloat16).reshape(tp_size, share_rows, model_width), 1
    )
    resid_own = lax.dynamic_slice_in_dim(resid, own_start, share_rows, 0)
    mixed_own = resid_own.astype(jnp.float32) + jnp.sum(proj_parts.astype(jnp.float32), axis=0)
    normed_own = (mixed_own * rms_scale(mixed_own, 1e-06) * ffn_gain).astype(jnp.bfloat16)
    normed_all = swap_tp(normed_own[None], 2).reshape(tok_rows, model_width)
    route_slots = routes.shape[1]
    capacity = max(2, 2 * tok_rows * route_slots // (seq_size * tp_size))
    tp_index = lax.axis_index("tp")
    group_experts = jnp.arange(seq_size, dtype=jnp.int32) * tp_size + tp_index
    named = routes[:, :, None] == group_experts[None, None, :]
    token_weight = jnp.sum(jnp.where(named, route_weight[:, :, None], 0.0), axis=1)
    is_named = jnp.any(named, axis=1)
    token_pos = jnp.arange(tok_rows, dtype=jnp.int32)
    earlier = (token_pos[None, :] < token_pos[:, None]).astype(jnp.bfloat16)
    rank = jnp.dot(earlier, is_named.astype(jnp.bfloat16), preferred_element_type=jnp.float32)
    place = jnp.where(is_named, rank.astype(jnp.int32), -1)
    slot_total = seq_size * capacity
    in_slot = place[:, :, None] == jnp.arange(capacity, dtype=jnp.int32)[None, None, :]
    pick = in_slot.reshape(tok_rows, slot_total).astype(jnp.bfloat16)
    combine = jnp.where(in_slot, token_weight[:, :, None], 0.0).reshape(tok_rows, slot_total)
    combine_high = lax.reduce_precision(combine, 8, 7)
    combine_low = (combine - combine_high).astype(jnp.bfloat16)
    outgoing = lax.dot_general(
        pick, normed_all, (((0,), (0,)), ((), ())), preferred_element_type=jnp.float32
    ).astype(jnp.bfloat16).reshape(seq_size, capacity, model_width)
    arrived = lax.all_to_all(outgoing, "sp", split_axis=0, concat_axis=0, tiled=True)
    item_count = arrived.shape[1]
    flat_rows = arrived.reshape(seq_size * item_count, model_width)
    gate_part = jnp.dot(flat_rows, expert_gate[0], preferred_element_type=jnp.float32)
    up_part = jnp.dot(flat_rows, expert_up[0], preferred_element_type=jnp.float32)
    hidden = (jax.nn.silu(gate_part) * up_part).astype(jnp.bfloat16)
    result = jnp.dot(hidden, expert_down[0], preferred_element_type=jnp.float32).astype(
        jnp.bfloat16
    )
    returned = lax.all_to_all(
        result.reshape(seq_size, item_count, model_width),
        "sp",
        split_axis=0,
        concat_axis=0,
        tiled=True,
    )
    returned_flat = returned.reshape(slot_total, model_width)
    routed = jnp.dot(
        combine_high.astype(jnp.bfloat16), returned_flat, preferred_element_type=jnp.float32
    ) + jnp.dot(combine_low, returned_flat, preferred_element_type=jnp.float32)
    shared_act = (
        jax.nn.silu(jnp.dot(normed_all, shared_gate, preferred_element_type=jnp.float32))
        * jnp.dot(normed_all, shared_up, preferred_element_type=jnp.float32)
    ).astype(jnp.bfloat16)
    shared_out = jnp.dot(shared_act, shared_down, preferred_element_type=jnp.float32)
    ffn_parts = swap_tp(
        (routed + shared_out).astype(jnp.bfloat16).reshape(tp_size, share_rows, model_width), 3
    )
    ffn_own = jnp.sum(ffn_parts.astype(jnp.float32), axis=0)
    return (mixed_own + ffn_own).astype(jnp.bfloat16)


def solution(mesh):
    placed = (
        P("sp", None),
        P("sp", "tp"),
        P("sp", "tp"),
        P("sp", "tp"),
        P("sp", "tp"),
        P("sp", "tp"),
        P("sp"),
        P("tp"),
        P(),
        P("tp", None),
        P(),
        P("sp", None),
        P("sp", None),
        P(("sp", "tp"), None, None),
        P(("sp", "tp"), None, None),
        P(("sp", "tp"), None, None),
        P(None, "tp"),
        P(None, "tp"),
        P("tp", None),
    )
    return jax.shard_map(
        local, mesh=mesh, in_specs=placed, out_specs=P(("sp", "tp"), None), check_vma=False
    )
```
